32 devices in a mesh: grp: 2 (over x), ep: 16 (over z, y, core).
Axes of the slice: x: 2, y: 2, z: 4, core: 2. Of those that a mesh axis runs over, the one named last changes fastest.
Arguments:
- hidden: bfloat16 [224, 2048], P(('grp', 'ep')), parts along dimension 0, may hold values from -6 to 6
- state_in: float32 [224, 64, 4096], P(('grp', 'ep')), parts along dimension 0, may hold values from -4 to 4
- conv_state: bfloat16 [224, 3, 4608], P(('grp', 'ep')), parts along dimension 0, may hold values from -6 to 6
- expert_ids: int32 [224, 4], P(('grp', 'ep')), parts along dimension 0, may hold values from 0 to 15, as said below
- group_prob: float32 [224], P(('grp', 'ep')), parts along dimension 0, may hold values from 0.25 to 1
- expert_score: float32 [224, 4], P(('grp', 'ep')), parts along dimension 0, may hold values from 0.05 to 1
- first_gain: bfloat16 [2048], replicated, may hold values from 0.099609375 to 1.8984375
- z_weight: bfloat16 [2048, 4096], P(None, 'ep'), may hold values from -0.125 to 0.125
- x_weight: bfloat16 [2048, 4096], P(None, 'ep'), may hold values from -0.125 to 0.125
- b_weight: bfloat16 [2048, 256], replicated, may hold values from -0.125 to 0.125
- c_weight: bfloat16 [2048, 256], replicated, may hold values from -0.125 to 0.125
- dt_weight: bfloat16 [2048, 64], replicated, may hold values from -0.125 to 0.125
- conv_weight: bfloat16 [4, 4608], replicated, may hold values from -3 to 3
- conv_bias: bfloat16 [4608], replicated, may hold values from -3 to 3
- dt_bias: float32 [64], replicated, may hold values from -4 to 0
- decay_log: float32 [64], replicated, may hold values from 0 to 2
- skip_gain: float32 [64], replicated, may hold values from 0.1 to 1.9
- inner_gain: bfloat16 [4096], replicated, may hold values from 0.099609375 to 1.8984375
- out_weight: bfloat16 [4096, 2048], P(None, 'ep'), may hold values from -0.09375 to 0.09375
- second_gain: bfloat16 [2048], replicated, may hold values from 0.099609375 to 1.8984375
- expert_gate: bfloat16 [16, 2048, 512], P('ep'), may hold values from -0.125 to 0.125
- expert_up: bfloat16 [16, 2048, 512], P('ep'), may hold values from -0.125 to 0.125
- expert_down: bfloat16 [16, 512, 2048], P('ep'), may hold values from -0.25 to 0.25
Outputs:
- layer_out: bfloat16 [224, 2048], P(('grp', 'ep')), parts along dimension 0
- state_out: float32 [224, 64, 4096], P(('grp', 'ep')), parts along dimension 0
- conv_out: bfloat16 [224, 3, 4608], P(('grp', 'ep')), parts along dimension 0
The draws below stay inside these ranges and needn't reach their ends.
There are 2 independent parts, one for each index of `grp`. The reference program is written for one: setup_inputs(seed, part) draws one part's arguments, and reference() takes and returns one part's arrays. A program takes and returns all parts, laid end to end along the dimension named above; an argument that names none is the same for every part. Nothing has to cross between parts.
Inputs may be any that keep to these rules, and one draw needn't show every extreme that they name: `expert_ids`: each row names 4 different experts of one expert group (numbers g * 8 to g * 8 + 7). Among the 7 rows of one device no expert is named more than 3 times, and in every draw one expert is named exactly 3 times by the rows of every device.
All inputs are finite; a program needn't handle non-finite values.
Results may differ from the reference program's by a relative error of at most 0.014.
Values may be sent and summed in bfloat16 or wider, within the bound.
A program may use at most 128 MiB of HBM per device.

```python
import math
import jax
import jax.numpy as jnp
from jax import lax

D = 2048
HEADS = 64
HEAD_DIM = 64
SSM_GROUPS = 4
STATE = 64
CONV = 4
MOE_HIDDEN = 512
EXP_GROUP = 8
TOP = 4
SEQ_DEV = 7
INNER = 4096
CONV_DIM = 4608
EXPERTS = 16
TOKENS = 112
CAP = 3
N_EP = 16


def draw_expert_ids(key, part):
    group_count = N_EP // EXP_GROUP
    hot_rows = min(SEQ_DEV, CAP + CAP * (EXP_GROUP - TOP) // TOP)
    hot_key, rest_key = jax.random.split(jax.random.fold_in(key, 11))
    hot_expert = jax.random.randint(hot_key, (), 0, N_EP)
    hot_group = hot_expert // EXP_GROUP
    hot_local = hot_expert % EXP_GROUP
    row_index = jnp.arange(SEQ_DEV, dtype=jnp.int32)[:, None]
    pick_index = jnp.arange(TOP, dtype=jnp.int32)[None, :]

    def one_block(block_key):
        key_order, key_inner, key_hot, key_shuffle, key_within = jax.random.split(block_key, 5)
        group_order = jax.random.permutation(key_order, group_count)
        sort_keys = (group_order == hot_group).astype(jnp.int32) * group_count + jnp.arange(group_count, dtype=jnp.int32)
        other_groups = group_order[jnp.argsort(sort_keys)][:group_count - 1]
        inner_keys = jax.random.split(key_inner, group_count - 1)
        inner_perm = jax.vmap(lambda one_key: jax.random.permutation(one_key, EXP_GROUP))(inner_keys)
        hot_perm = jax.random.permutation(key_hot, EXP_GROUP - 1)
        early_place = jnp.where(pick_index == 0, 0, 1 + (row_index * (TOP - 1) + pick_index - 1) % (EXP_GROUP - 1))
        late_place = 1 + (CAP * (TOP - 1) + (row_index - CAP) * TOP + pick_index) % (EXP_GROUP - 1)
        hot_place = jnp.where(row_index < CAP, early_place, late_place)
        hot_local_pick = jnp.where(hot_place == 0, hot_local, (hot_local + 1 + hot_perm[jnp.maximum(hot_place - 1, 0)]) % EXP_GROUP)
        hot_pick = hot_group * EXP_GROUP + hot_local_pick
        cold_row = jnp.maximum(row_index - hot_rows, 0)
        cold_group = cold_row % (group_count - 1)
        cold_turn = cold_row // (group_count - 1)
        cold_place = (cold_turn * TOP + pick_index) % EXP_GROUP
        cold_pick = other_groups[cold_group] * EXP_GROUP + inner_perm[cold_group, cold_place]
        block_ids = jnp.where(row_index < hot_rows, hot_pick, cold_pick)
        shuffle = jax.random.permutation(key_shuffle, SEQ_DEV)
        block_ids = block_ids[shuffle]
        within_keys = jax.random.split(key_within, SEQ_DEV)
        within = jax.vmap(lambda one_key: jax.random.permutation(one_key, TOP))(within_keys)
        return jnp.take_along_axis(block_ids, within, axis=1)
    block_keys = jax.random.split(rest_key, N_EP)
    return jax.vmap(one_block)(block_keys).reshape(N_EP * SEQ_DEV, TOP).astype(jnp.int32)


def block_levels(key, extent, cuts, least, high):
    level = 1.0
    for dim, blocks in cuts:
        heights = jax.random.uniform(jax.random.fold_in(jax.random.fold_in(key, 6), dim), (blocks,), jnp.float32, least / len(cuts), high / len(cuts))
        level = level * jnp.repeat(jnp.exp(heights), extent[dim] // blocks).reshape((-1,) + (1,) * (len(extent) - 1 - dim))
    return level


def normal_values(own_key, shape, width, limit, pieces=(), kind=jnp.bfloat16):
    loudness = block_levels(own_key, shape, pieces, -0.22, 0.18) if pieces else 1.0
    result = jax.random.normal(own_key, shape, jnp.float32) * width * loudness
    return jnp.minimum(jnp.maximum(result, -limit), limit).astype(kind)


def setup_inputs(seed: int = 0, part: int = 0) -> dict:
    key_list = jax.random.split(jax.random.key(seed), 24)
    part_splits = jax.random.split(jax.random.fold_in(key_list[23], part), 24)
    return {
        "hidden": normal_values(part_splits[0], (TOKENS, D), 1.0, 6.0, ((0, 16),)),
        "state_in": normal_values(part_splits[1], (TOKENS, HEADS, HEAD_DIM * STATE), 0.3, 4.0, ((0, 16),), jnp.float32),
        "conv_state": normal_values(part_splits[2], (TOKENS, CONV - 1, CONV_DIM), 1.0, 6.0, ((0, 16),)),
        "expert_ids": draw_expert_ids(jax.random.fold_in(jax.random.fold_in(key_list[23], part), 71), part),
        "group_prob": jnp.clip(jnp.exp(math.log(1.0) - 1.3862944 * jax.random.uniform(part_splits[4], (TOKENS,), jnp.float32) ** block_levels(part_splits[4], (TOKENS,), ((0, 16),), -0.2, 0.2)), 0.25, 1.0),
        "expert_score": jnp.clip(jnp.exp(math.log(1.0) - 2.9957323 * jax.random.uniform(part_splits[5], (TOKENS, TOP), jnp.float32) ** block_levels(part_splits[5], (TOKENS, TOP), ((0, 16),), -0.2, 0.2)), 0.05, 1.0),
        "first_gain": jnp.clip(1.0 + 0.18 * jax.random.normal(key_list[6], (D,), jnp.float32), 0.099609375, 1.8984375).astype(jnp.bfloat16),
        "z_weight": normal_values(key_list[7], (D, INNER), D ** -0.5, 0.125, ((1, 16),)),
        "x_weight": normal_values(key_list[8], (D, INNER), D ** -0.5, 0.125, ((1, 16),)),
        "b_weight": normal_values(key_list[9], (D, SSM_GROUPS * STATE), D ** -0.5, 0.125),
        "c_weight": normal_values(key_list[10], (D, SSM_GROUPS * STATE), D ** -0.5, 0.125),
        "dt_weight": normal_values(key_list[11], (D, HEADS), D ** -0.5, 0.125),
        "conv_weight": normal_values(key_list[12], (CONV, CONV_DIM), 0.5, 3.0),
        "conv_bias": normal_values(key_list[13], (CONV_DIM,), 0.5, 3.0),
        "dt_bias": jnp.clip(jax.random.uniform(key_list[14], (HEADS,), jnp.float32, -4.0, 0.0), -4.0, 0.0),
        "decay_log": jnp.clip(jax.random.uniform(key_list[15], (HEADS,), jnp.float32, 0.0, 2.0), 0.0, 2.0),
        "skip_gain": jnp.clip(1.0 + 0.18 * jax.random.normal(key_list[16], (HEADS,), jnp.float32), 0.1, 1.9),
        "inner_gain": jnp.clip(1.0 + 0.18 * jax.random.normal(key_list[17], (INNER,), jnp.float32), 0.099609375, 1.8984375).astype(jnp.bfloat16),
        "out_weight": normal_values(key_list[18], (INNER, D), INNER ** -0.5, 0.09375, ((1, 16),)),
        "second_gain": jnp.clip(1.0 + 0.18 * jax.random.normal(key_list[19], (D,), jnp.float32), 0.099609375, 1.8984375).astype(jnp.bfloat16),
        "expert_gate": normal_values(key_list[20], (EXPERTS, D, MOE_HIDDEN), D ** -0.5, 0.125, ((0, 16),)),
        "expert_up": normal_values(key_list[21], (EXPERTS, D, MOE_HIDDEN), D ** -0.5, 0.125, ((0, 16),)),
        "expert_down": normal_values(key_list[22], (EXPERTS, MOE_HIDDEN, D), MOE_HIDDEN ** -0.5, 0.25, ((0, 16),)),
    }


EPS = 1e-06

def rms_scale(values, gain_vec):
    return values * lax.rsqrt(lax.optimization_barrier(jnp.mean(values * values, axis=-1, keepdims=True)) + EPS) * gain_vec.astype(jnp.float32)

def state_step(active, dt_raw, state_in, dt_bias, decay_log, skip_gain):
    row_count = active.shape[0]
    inner_width = HEADS * HEAD_DIM
    state_span = SSM_GROUPS * STATE
    per_group = HEADS // SSM_GROUPS
    x_heads = active[:, :inner_width].reshape(row_count, HEADS, HEAD_DIM)
    b_input = active[:, inner_width:inner_width + state_span].reshape(row_count, SSM_GROUPS, STATE)
    c_input = active[:, inner_width + state_span:].reshape(row_count, SSM_GROUPS, STATE)
    b_heads = jnp.repeat(b_input, per_group, axis=1)
    c_heads = jnp.repeat(c_input, per_group, axis=1)
    step_size = jax.nn.softplus(dt_raw.astype(jnp.float32) + dt_bias[None, :])
    decay_rate = jnp.exp(-step_size * jnp.exp(decay_log)[None, :])
    carried = state_in.reshape(row_count, HEADS, HEAD_DIM, STATE)
    carried = decay_rate[:, :, None, None] * carried + (step_size[:, :, None] * x_heads)[:, :, :, None] * b_heads[:, :, None, :]
    readout = jnp.einsum('bhpn,bhn->bhp', carried, c_heads, precision=lax.Precision.HIGHEST)
    readout = readout + skip_gain[None, :, None] * x_heads
    return (readout.reshape(row_count, inner_width), carried.reshape(row_count, HEADS, HEAD_DIM * STATE))

def reference(hidden, state_in, conv_state, expert_ids, group_prob, expert_score, first_gain, z_weight, x_weight, b_weight, c_weight, dt_weight, conv_weight, conv_bias, dt_bias, decay_log, skip_gain, inner_gain, out_weight, second_gain, expert_gate, expert_up, expert_down):
    row_count = hidden.shape[0]
    normed = rms_scale(hidden.astype(jnp.float32), first_gain).astype(jnp.bfloat16)
    gate_z = jnp.dot(normed, z_weight, preferred_element_type=jnp.float32).astype(jnp.bfloat16)
    x_part = jnp.dot(normed, x_weight, preferred_element_type=jnp.float32).astype(jnp.bfloat16)
    b_part = jnp.dot(normed, b_weight, preferred_element_type=jnp.float32).astype(jnp.bfloat16)
    c_part = jnp.dot(normed, c_weight, preferred_element_type=jnp.float32).astype(jnp.bfloat16)
    dt_raw = jnp.dot(normed, dt_weight, preferred_element_type=jnp.float32).astype(jnp.bfloat16)
    fresh_input = jnp.concatenate([x_part, b_part, c_part], axis=1)
    window = jnp.concatenate([conv_state, fresh_input[:, None, :]], axis=1)
    summed = lax.optimization_barrier(jnp.sum(window.astype(jnp.float32) * conv_weight.astype(jnp.float32)[None], axis=1))
    active = jax.nn.silu(summed + conv_bias.astype(jnp.float32)[None, :])
    readout, state_out = state_step(active, dt_raw, state_in, dt_bias, decay_log, skip_gain)
    gated = readout * jax.nn.silu(gate_z.astype(jnp.float32))
    y_mix = rms_scale(gated, inner_gain).astype(jnp.bfloat16)
    projected = jnp.dot(y_mix, out_weight, preferred_element_type=jnp.float32).astype(jnp.bfloat16)
    projected = lax.optimization_barrier(projected)
    mixed_rows = (hidden.astype(jnp.float32) + projected.astype(jnp.float32)).astype(jnp.bfloat16)
    normed2 = rms_scale(mixed_rows.astype(jnp.float32), second_gain).astype(jnp.bfloat16)
    route_share = group_prob[:, None] * expert_score / lax.optimization_barrier(jnp.sum(expert_score, axis=1, keepdims=True))
    flat_ids = expert_ids.reshape(-1).astype(jnp.int32)
    flat_share = route_share.reshape(-1)
    route_count = flat_ids.shape[0]
    flat_rows = jnp.repeat(jnp.arange(row_count, dtype=jnp.int32), TOP)
    max_rows = N_EP * CAP

    def per_expert(accum, expert):
        is_routed = (flat_ids == expert).astype(jnp.int32)
        sort_keys = (1 - is_routed) * route_count + jnp.arange(route_count, dtype=jnp.int32)
        chosen = jnp.argsort(sort_keys)[:max_rows].astype(jnp.int32)
        token_rows = flat_rows[chosen]
        picked = normed2[token_rows]
        gate_part = jnp.dot(picked, expert_gate[expert], preferred_element_type=jnp.float32)
        up_part = jnp.dot(picked, expert_up[expert], preferred_element_type=jnp.float32)
        hidden_act = (jax.nn.silu(gate_part) * up_part).astype(jnp.bfloat16)
        expert_out = jnp.dot(hidden_act, expert_down[expert], preferred_element_type=jnp.float32).astype(jnp.bfloat16)
        expert_out = lax.optimization_barrier(expert_out)
        weight_vec = flat_share[chosen] * is_routed[chosen].astype(jnp.float32)
        accum = accum.at[token_rows].add(weight_vec[:, None] * expert_out.astype(jnp.float32))
        return (accum, None)
    blank = jnp.zeros((row_count, hidden.shape[1]), jnp.float32)
    moe_sum, _ = lax.scan(per_expert, blank, jnp.arange(EXPERTS, dtype=jnp.int32))
    layer_out = (mixed_rows.astype(jnp.float32) + moe_sum).astype(jnp.bfloat16)
    return (layer_out, state_out, window[:, 1:, :])
```

```python
import functools

import jax
import jax.numpy as jnp
from jax import lax
from jax.experimental import pallas as pl
from jax.experimental.pallas import tpu as pltpu
from jax.sharding import PartitionSpec as P

HEADS = 64
HEAD_DIM = 64
SSM_GROUPS = 4
STATE = 64
TOP = 4
EPS = 1e-06
MESH = pl.DeviceIdType.MESH
F32 = jnp.float32
BF16 = jnp.bfloat16
ROWS = 8
INNER = HEADS * HEAD_DIM
SPAN = SSM_GROUPS * STATE


def rms_scale(values, gain_vec):
    return (
        values
        * lax.rsqrt(jnp.mean(values * values, axis=-1, keepdims=True) + EPS)
        * gain_vec.astype(F32)
    )


def dot(a, b):
    return jnp.dot(a, b, preferred_element_type=F32)


def dot_nt(a, b):
    return lax.dot_general(a, b, (((1,), (1,)), ((), ())), preferred_element_type=F32)


def iota(shape, axis):
    return lax.broadcasted_iota(jnp.int32, shape, axis)


def onehot(mask):
    return mask.astype(F32).astype(BF16)


def peer(index):
    return (lax.axis_index("grp"), index)


def remote(src, dst, send_sem, recv_sem, index):
    return pltpu.make_async_remote_copy(
        src_ref=src,
        dst_ref=dst,
        send_sem=send_sem,
        recv_sem=recv_sem,
        device_id=peer(index),
        device_id_type=MESH,
    )


def spread(ref):
    value = ref[...].astype(F32)
    return jnp.concatenate([value[i : i + 1] for i in range(value.shape[0])], axis=1)


def column(row):
    size = row.shape[1]
    at = iota((size, size), 0)
    to = iota((size, size), 1)
    return jnp.sum(jnp.where(at == to, row, jnp.zeros_like(row)), axis=1, keepdims=True)


class Gather:
    def __init__(self, n, buf, send, recv):
        self.n, self.buf, self.send, self.recv = n, buf, send, recv
        self.me = lax.axis_index("ep")
        self.outer = n // 4
        core = lax.rem(self.me, 2)
        mid = lax.rem(self.me // 2, 2)
        self.mate = self.me + 1 - 2 * core
        self.across = self.me + 2 - 4 * mid

    def go(self, src, block, kind, d, to):
        sem = self.recv.at[kind * self.outer + d]
        remote(src, self.buf.at[block], self.send.at[0], sem, to).start()

    def arrive(self, block, kind, d):
        sem = self.recv.at[kind * self.outer + d]
        piece = self.buf.at[block]
        remote(piece, piece, self.send.at[0], sem, self.mate).wait_recv()

    def start(self, src):
        for d in range(1, self.outer):
            self.go(src, self.me, 0, d, lax.rem(self.me + 4 * d, self.n))
        self.go(src, self.me, 1, 0, self.across)
        self.go(src, self.me, 2, 0, self.mate)

    def near(self, d):
        return lax.rem(self.me + self.n - 4 * d, self.n)

    def far(self, d):
        return lax.rem(self.across + self.n - 4 * d, self.n)

    def middle(self):
        for d in range(1, self.outer):
            block = self.near(d)
            self.arrive(block, 0, d)
            self.go(self.buf.at[block], block, 1, d, self.across)
            self.go(self.buf.at[block], block, 2, d, self.mate)

    def last(self):
        for d in range(self.outer):
            block = self.far(d)
            self.arrive(block, 1, d)
            self.go(self.buf.at[block], block, 3, d, self.mate)

    def finish(self):
        for kind in (2, 3):
            for d in range(self.outer):
                self.arrive(self.me, kind, d)

    def drain(self):
        piece = self.buf.at[pl.ds(0, self.n - 1)]
        remote(piece, piece, self.send.at[0], self.recv.at[0], self.mate).wait_send()


class Exchange:
    def __init__(self, n, out_buf, in_buf, send, recv):
        self.n, self.out_buf, self.in_buf, self.send, self.recv = n, out_buf, in_buf, send, recv
        self.me = lax.axis_index("ep")

    def start(self):
        for d in range(1, self.n):
            to = lax.rem(self.me + d, self.n)
            remote(
                self.out_buf.at[to], self.in_buf.at[self.me], self.send.at[0], self.recv.at[0], to
            ).start()
        self.in_buf[self.me] = self.out_buf[self.me]

    def _all(self):
        part = pl.ds(0, self.n - 1)
        return remote(
            self.out_buf.at[part], self.in_buf.at[part], self.send.at[0], self.recv.at[0], self.me
        )

    def wait(self):
        self._all().wait_recv()

    def drain(self):
        self._all().wait_send()


def mixer_kernel(n, cap, *refs):
    (
        own_ref,
        ids_ref,
        prob_ref,
        score_ref,
        conv_ref,
        taps_ref,
        bias_ref,
        g1_ref,
        gi_ref,
        g2_ref,
        dtb_ref,
        dlog_ref,
        skip_ref,
        z_any,
        x_any,
        b_any,
        c_any,
        dt_any,
        ow_any,
        eg_any,
        eu_any,
        ed_any,
        st_any,
        out_ref,
        sx_ref,
        decx_ref,
        bc_ref,
        fresh_ref,
        hid,
        hbuf,
        hall,
        hg,
        hsq,
        zw,
        xw,
        bw,
        cw,
        dw,
        ow,
        eg,
        eu,
        ed,
        st,
        prod,
        fold,
        r0s,
        stepx,
        cpart,
        pre_out,
        pre_in,
        x_out,
        x_in,
        yown,
        ybuf,
        sel,
        bigh,
        bigl,
        hsel,
        p_out,
        p_in,
        mg,
        stage,
        spot_rows,
        o_out,
        o_in,
        wsem,
        gs,
        gr,
        as_,
        ar,
    ) = refs
    rows, width = own_ref.shape
    cols = zw.shape[1]
    ncol = ow.shape[1]
    total = n * ROWS
    slots = n * cap
    sp = sel.shape[0] // n
    chunks = width // 128
    per = HEADS // SSM_GROUPS
    me = lax.axis_index("ep")

    pairs = [(b_any, bw), (c_any, cw), (dt_any, dw)]
    pairs += [(st_any.at[t], st.at[t]) for t in range(rows)]
    pairs += [(x_any, xw), (z_any, zw), (ow_any, ow)]
    pairs += [(eg_any.at[0], eg), (eu_any.at[0], eu), (ed_any.at[0], ed)]
    loads = [pltpu.make_async_copy(src, dst, wsem.at[i]) for i, (src, dst) in enumerate(pairs)]
    for load in loads:
        load.start()

    barrier = pltpu.get_barrier_semaphore()
    for d in range(1, n):
        pl.semaphore_signal(
            barrier, inc=1, device_id=peer(lax.rem(me + d, n)), device_id_type=MESH
        )
    ids = ids_ref[...].astype(F32)
    pick = iota((TOP, 128), 0)
    lane = iota((TOP, 128), 1)
    spot = jnp.zeros((TOP, 128), F32)
    for r in range(rows):
        spot = spot + jnp.where(lane == TOP * r + pick, ids[:, r : r + 1] + 1.0, 0.0)
    id_row = jnp.sum(spot, axis=0, keepdims=True) - 1.0
    id_row = jnp.concatenate([id_row, jnp.full((1, width - 128), -1.0, F32)], axis=1)
    hid[...] = jnp.concatenate([own_ref[...].astype(F32), id_row], axis=0).astype(BF16)
    pl.semaphore_wait(barrier, n - 1)

    hidden_ag = Gather(n, hbuf, gs.at[pl.ds(0, 1)], gr.at[pl.ds(0, n)])
    hidden_ag.start(hid)
    hbuf[me] = hid[...]

    gain1 = spread(g1_ref)
    own = hid[...].astype(F32)
    mine = rms_scale(own, gain1).astype(BF16)
    taps = taps_ref[...].astype(F32)
    held = conv_ref.shape[0]
    summed = spread(bias_ref)
    for k in range(held):
        summed = summed + conv_ref[k].astype(F32) * taps[k : k + 1]
    cpart[...] = jnp.concatenate([summed, jnp.zeros((ROWS - rows, summed.shape[1]), F32)], axis=0)
    for load in loads[:3]:
        load.wait()
    fresh_b = dot(mine, bw[...]).astype(BF16)
    fresh_c = dot(mine, cw[...]).astype(BF16)
    fresh_ref[:, INNER : INNER + SPAN] = fresh_b
    fresh_ref[:, INNER + SPAN :] = fresh_c
    b_act = jax.nn.silu(
        cpart[:, INNER : INNER + SPAN]
        + fresh_b.astype(F32) * taps[held : held + 1, INNER : INNER + SPAN]
    )
    c_act = jax.nn.silu(
        cpart[:, INNER + SPAN :] + fresh_c.astype(F32) * taps[held : held + 1, INNER + SPAN :]
    )
    bc_ref[:, :SPAN] = b_act
    bc_ref[:, SPAN:] = c_act
    dt = dot_nt(mine, dw[...]).astype(BF16).astype(F32)
    step = jax.nn.softplus(dt + dtb_ref[...])
    dt_t = dot_nt(dw[...], mine).astype(BF16).astype(F32)
    step_t = jax.nn.softplus(dt_t + column(dtb_ref[...]))
    decay_t = jnp.exp(-step_t * jnp.exp(column(dlog_ref[...])))
    for t in range(rows):
        at = slice(t * HEADS, (t + 1) * HEADS)
        stepx[at, :] = jnp.broadcast_to(step_t[:, t : t + 1], (HEADS, 128))
        decx_ref[at, :] = jnp.broadcast_to(decay_t[:, t : t + 1], (HEADS, 128))
    pad = slice(rows * HEADS, ROWS * HEADS)
    stepx[pad, :] = jnp.zeros(((ROWS - rows) * HEADS, 128), F32)
    decx_ref[pad, :] = jnp.zeros(((ROWS - rows) * HEADS, 128), F32)
    r0s[pad, :] = jnp.zeros(((ROWS - rows) * HEADS, 128), F32)
    bc = b_act * c_act
    bc_hi = bc.astype(BF16)
    bc_lo = (bc - bc_hi.astype(F32)).astype(BF16)
    group = onehot(iota((SPAN, 128), 0) // STATE == iota((SPAN, 128), 1) // per)
    inner = dot(bc_hi, group) + dot(bc_lo, group)
    coef = step * inner[:, :HEADS] + skip_ref[...]
    row_ok = iota((ROWS, HEADS), 0) < rows
    coef = jnp.where(row_ok, coef, 0.0)
    coef = jnp.concatenate([coef, jnp.zeros((ROWS, 128 - HEADS), F32)], axis=1).astype(BF16)

    hidden_ag.middle()

    def make_fold(i, carry):
        at = pl.ds(pl.multiple_of(i * 256, 256), 256)
        p_of = iota((256, 128), 0) // STATE + 4 * i
        fold[at, :] = onehot(p_of == lax.rem(iota((256, 128), 1), HEAD_DIM))
        return carry

    lax.fori_loop(0, INNER // 256, make_fold, 0)

    def make_prod(t, carry):
        pltpu.make_async_copy(st_any.at[t], st.at[t], wsem.at[3 + t]).wait()
        row = bc_ref[pl.ds(t, 1), :]
        cs = []
        for g in range(SSM_GROUPS):
            c = row[:, SPAN + g * STATE : SPAN + (g + 1) * STATE]
            cs.append(jnp.broadcast_to(jnp.concatenate([c, c], axis=1), (per, 2 * STATE)))
        c_all = jnp.concatenate(cs, axis=0)
        at = pl.ds(pl.multiple_of(t * HEADS, HEADS), HEADS)
        for k in range(HEAD_DIM * STATE // 128):
            lanes = slice(k * 128, (k + 1) * 128)
            prod[at, lanes] = (st[t, :, lanes] * c_all).astype(BF16)
        return carry

    lax.fori_loop(0, rows, make_prod, 0)
    r0 = dot(prod[...], fold[...])
    r0s[: rows * HEADS, :] = r0 * decx_ref[: rows * HEADS, :]
    low_half = iota((ROWS, 128), 1) < HEAD_DIM
    for m in range(INNER // 128):
        even = r0s[pl.ds(2 * m, ROWS, stride=HEADS), :]
        odd = r0s[pl.ds(2 * m + 1, ROWS, stride=HEADS), :]
        j, off = (m * 128) // cols, (m * 128) % cols
        pre_out[j, :, off : off + 128] = jnp.where(low_half, even, odd).astype(BF16)
    for j in range(n):
        pre_out[j, :, cols : 2 * cols] = cpart[:, j * cols : (j + 1) * cols].astype(BF16)
        pre_out[j, :, 2 * cols :] = coef
    pre = Exchange(n, pre_out, pre_in, as_.at[pl.ds(0, 1)], ar.at[pl.ds(0, 1)])
    pre.start()

    hidden_ag.last()
    hidden_ag.finish()
    for j in range(0, n, 2):
        at = slice(j * ROWS, (j + 2) * ROWS)
        pair = jnp.concatenate([hbuf[j].astype(F32), hbuf[j + 1].astype(F32)], axis=0)
        hall[at, :] = pair.astype(BF16)
        hg[at, :] = (pair * gain1).astype(BF16)
        hsq[at, :] = (pair * pair).astype(BF16)
    for load in loads[3 + rows : 5 + rows]:
        load.wait()
    ones = jnp.ones((width, 128), BF16)
    scale = lax.rsqrt(dot(hsq[...], ones) * (1.0 / width) + EPS)
    scale = jnp.concatenate([scale] * (cols // 128), axis=1)
    xp = (dot(hg[...], xw[...]) * scale).astype(BF16).astype(F32)
    zp = (dot(hg[...], zw[...]) * scale).astype(BF16).astype(F32)
    for j in range(n):
        x_out[j] = xp[j * ROWS : (j + 1) * ROWS].astype(BF16)
    my_cols = pl.ds(pl.multiple_of(me * cols, 128), cols)
    tap = taps_ref[:, my_cols].astype(F32)[held : held + 1]
    gain_all = spread(gi_ref)
    cpart_gain = jnp.broadcast_to(gain_all, (ROWS, INNER))
    stage[pl.ds(0, ROWS), :] = cpart_gain[:, :width]
    stage[pl.ds(ROWS, ROWS), :] = cpart_gain[:, width:]
    half_n = n // 2
    upper = me // half_n
    gain_cols = stage[
        pl.ds(pl.multiple_of(upper * ROWS, ROWS), ROWS),
        pl.ds(pl.multiple_of(lax.rem(me, half_n) * cols, 128), cols),
    ]
    pre.wait()
    for j in range(0, n, 2):
        ys = []
        for i in (j, j + 1):
            at = slice(i * ROWS, (i + 1) * ROWS)
            block = pre_in[i].astype(F32)
            xa = jax.nn.silu(block[:, cols : 2 * cols] + xp[at] * tap)
            packed = block[:, 2 * cols :]
            grown = []
            for k in range(cols // 128):
                index = (me * cols + k * 128) // HEAD_DIM + iota((ROWS, 128), 1) // HEAD_DIM
                grown.append(jnp.take_along_axis(packed, index, axis=1))
            readout = block[:, :cols] + jnp.concatenate(grown, axis=1) * xa
            ys.append(readout * jax.nn.silu(zp[at]) * gain_cols)
        yown[j * ROWS : (j + 2) * ROWS, :] = jnp.concatenate(ys, axis=0).astype(BF16)

    y_ag = Gather(n, ybuf, gs.at[pl.ds(1, 1)], gr.at[pl.ds(n, n)])
    y_ag.start(yown)
    back = Exchange(n, x_out, x_in, as_.at[pl.ds(1, 1)], ar.at[pl.ds(1, 1)])
    back.start()
    ybuf[me] = yown[...]

    q = iota((slots, total), 0)
    t_of = iota((slots, total), 1)
    last = onehot(t_of == lax.rem(q, n) * ROWS + (ROWS - 1))
    id_all = dot(last, hall[:, :128])
    f_lane = iota((128, total), 0) // TOP
    token = lax.rem(iota((128, total), 1), ROWS)
    m_here = onehot(f_lane == token)
    m_less = onehot(f_lane < token)
    flags = jnp.concatenate([onehot(id_all == float(e)) for e in range(n)], axis=0)
    here = dot(flags, m_here)
    before = dot(flags, m_less)
    same = lax.rem(q, n) == t_of // ROWS
    rank_q = (q // n).astype(F32)
    own_row = iota((ROWS, total), 0)
    own_col = iota((ROWS, total), 1)
    for e in range(n):
        at = slice(e * slots, (e + 1) * slots)
        chosen = same & (here[at] > 0.5) & (before[at] == rank_q)
        tail = [(own_col == e * ROWS + own_row).astype(F32)]
        if sp > slots + ROWS:
            tail.append(jnp.zeros((sp - slots - ROWS, total), F32))
        sel[e * sp : (e + 1) * sp, :] = jnp.concatenate(
            [chosen.astype(F32)] + tail, axis=0
        ).astype(BF16)

    y_ag.middle()

    span = chunks * cap
    wide = n * span
    col = iota((rows, wide), 1).astype(F32)
    e_of = jnp.floor((col + 0.5) * (1.0 / span))
    in_e = col - e_of * span
    k_of = jnp.floor((in_e + 0.5) * (1.0 / cap))
    r_of = in_e - k_of * cap
    score = score_ref[...]
    share = prob_ref[...] * score / jnp.sum(score, axis=0, keepdims=True)
    weight = jnp.zeros((rows, wide), F32)
    used = jnp.zeros((rows, wide), F32)
    for i in range(TOP):
        hit = (column(ids[i : i + 1]) == e_of).astype(F32)
        used = used + hit
        weight = weight + hit * column(share[i : i + 1])
    row_id = iota((rows, wide), 0)
    rank = jnp.zeros((rows, wide), F32)
    for r in range(rows - 1):
        rank = rank + jnp.where(row_id > r, used[r : r + 1, :], 0.0)
    weight = jnp.where(rank == r_of, weight, 0.0)
    weight = jnp.concatenate([weight, jnp.zeros((ROWS - rows, wide), F32)], axis=0)
    k_row = k_of[0:1]
    for k in range(0, chunks, 2):
        both = jnp.concatenate(
            [jnp.where(k_row == float(k + i), weight, 0.0) for i in range(2)], axis=0
        )
        high = both.astype(BF16)
        at = slice(k * ROWS, (k + 2) * ROWS)
        bigh[at, :] = high
        bigl[at, :] = (both - high.astype(F32)).astype(BF16)
    pick_me = sel[pl.ds(pl.multiple_of(me * sp, 16), sp), :][:slots]
    hsel[...] = dot(pick_me, hall[...])

    y_ag.last()

    back.wait()
    for j in range(n):
        xv = x_in[j]
        fresh_ref[:, j * cols : (j + 1) * cols] = xv
        at = slice(j * cols, (j + 1) * cols)
        xa = jax.nn.silu(cpart[:, at] + xv.astype(F32) * taps_ref[held : held + 1, at].astype(F32))
        for k in range(cols // 128):
            m = (j * cols) // 128 + k
            piece = xa[:, k * 128 : (k + 1) * 128]
            sx_ref[pl.ds(2 * m, ROWS, stride=HEADS), :] = piece
            sx_ref[pl.ds(2 * m + 1, ROWS, stride=HEADS), :] = pltpu.roll(piece, HEAD_DIM, 1)
    sx_ref[...] = sx_ref[...] * stepx[...]

    loads[5 + rows].wait()
    y_ag.finish()
    acc = jnp.zeros((total, ncol), F32)
    ssq = jnp.zeros((total, 128), F32)
    inv_gain = (1.0 / gain_all).astype(BF16)
    ones_c = jnp.ones((cols, 128), BF16)
    for j in range(n):
        at = slice(j * cols, (j + 1) * cols)
        yb = ybuf[j]
        acc = acc + dot(yb, ow[at, :])
        raw = yb * inv_gain[:, at]
        ssq = ssq + dot(raw * raw, ones_c)
    scale = lax.rsqrt(ssq * (1.0 / INNER) + EPS)
    p = (acc * scale[:, :ncol]).astype(BF16)
    picked = dot(sel[...], p).astype(BF16)
    for e in range(n):
        p_out[e] = picked[e * sp : e * sp + slots + ROWS]
    p_ex = Exchange(n, p_out, p_in, as_.at[pl.ds(2, 1)], ar.at[pl.ds(2, 1)])
    p_ex.start()
    gain2 = spread(g2_ref)
    for load in loads[6 + rows :]:
        load.wait()
    p_ex.wait()
    ssq = jnp.zeros((slots, 128), F32)
    ones_n = jnp.ones((ncol, 128), BF16)
    mixed = []
    for j in range(n):
        at = slice(j * ncol, (j + 1) * ncol)
        block = p_in[j].astype(F32)
        m = (hsel[:, at] + block[:slots]).astype(BF16).astype(F32)
        mg[:, at] = (m * gain2[:, at]).astype(BF16)
        ssq = ssq + dot((m * m).astype(BF16), ones_n)
        mixed.append((own[:, at] + block[slots:]).astype(BF16).astype(F32))
    mixed = jnp.concatenate(mixed, axis=1)
    scale = lax.rsqrt(ssq * (1.0 / width) + EPS)
    acts = []
    for j in range(0, eg.shape[1], 128):
        at = slice(j, j + 128)
        gate = dot(mg[...], eg[:, at]) * scale
        up = dot(mg[...], eu[:, at]) * scale
        acts.append((jax.nn.silu(gate) * up).astype(BF16))
    act = jnp.concatenate(acts, axis=1)
    for k in range(0, chunks, 2):
        part = dot(act, ed[:, k * 128 : (k + 2) * 128])
        for i in range(2):
            for r in range(cap):
                spot_rows[pl.ds((k + i) * cap + r, n, stride=span), :] = part[
                    r * n : (r + 1) * n, i * 128 : (i + 1) * 128
                ]
    for s in range(n):
        o_out[s] = spot_rows[s * span : (s + 1) * span, :].astype(BF16)
    o_ex = Exchange(n, o_out, o_in, as_.at[pl.ds(3, 1)], ar.at[pl.ds(3, 1)])
    o_ex.start()
    hidden_ag.drain()
    y_ag.drain()
    pre.drain()
    back.drain()
    p_ex.drain()
    o_ex.wait()
    got = jnp.concatenate([o_in[e] for e in range(n)], axis=0)
    moe = dot(bigh[...], got) + dot(bigl[...], got)
    for k in range(chunks):
        at = slice(k * 128, (k + 1) * 128)
        out_ref[:, at] = (mixed[:, at] + moe[k * ROWS : (k + 1) * ROWS])[:rows].astype(BF16)
    o_ex.drain()


def mixer(n, cap, args, rows, width, z_weight, out_weight, expert_gate, expert_down):
    cols = z_weight.shape[1]
    ncol = out_weight.shape[1]
    units = expert_gate.shape[2]
    total = n * ROWS
    slots = n * cap
    sp = (slots + ROWS + 15) // 16 * 16
    chunks = width // 128
    span = chunks * cap
    vm = pl.BlockSpec(memory_space=pltpu.VMEM)
    hbm = pl.BlockSpec(memory_space=pl.ANY)
    dma = pltpu.SemaphoreType.DMA

    def buf(*shape, dtype=BF16):
        return pltpu.VMEM(shape, dtype)

    return pl.pallas_call(
        functools.partial(mixer_kernel, n, cap),
        out_shape=(
            jax.ShapeDtypeStruct((rows, width), BF16),
            jax.ShapeDtypeStruct((ROWS * HEADS, 128), F32),
            jax.ShapeDtypeStruct((ROWS * HEADS, 128), F32),
            jax.ShapeDtypeStruct((ROWS, 2 * SPAN), F32),
            jax.ShapeDtypeStruct((ROWS, INNER + 2 * SPAN), BF16),
        ),
        in_specs=[vm] * 13 + [hbm] * 10,
        out_specs=(vm,) * 5,
        scratch_shapes=[
            buf(ROWS, width),
            buf(n, ROWS, width),
            buf(total, width),
            buf(total, width),
            buf(total, width),
            buf(width, cols),
            buf(width, cols),
            buf(width, SPAN),
            buf(width, SPAN),
            buf(HEADS, width),
            buf(INNER, ncol),
            buf(width, units),
            buf(width, units),
            buf(units, width),
            buf(rows, HEADS, HEAD_DIM * STATE, dtype=F32),
            buf(rows * HEADS, HEAD_DIM * STATE),
            buf(INNER, 128),
            buf(ROWS * HEADS, 128, dtype=F32),
            buf(ROWS * HEADS, 128, dtype=F32),
            buf(ROWS, INNER + 2 * SPAN, dtype=F32),
            buf(n, ROWS, 2 * cols + 128),
            buf(n, ROWS, 2 * cols + 128),
            buf(n, ROWS, cols),
            buf(n, ROWS, cols),
            buf(total, cols),
            buf(n, total, cols),
            buf(n * sp, total),
            buf(chunks * ROWS, n * span),
            buf(chunks * ROWS, n * span),
            buf(slots, width, dtype=F32),
            buf(n, slots + ROWS, ncol),
            buf(n, slots + ROWS, ncol),
            buf(slots, width),
            buf(2 * ROWS, width, dtype=F32),
            buf(n * span, 128, dtype=F32),
            buf(n, span, 128),
            buf(n, span, 128),
            dma((9 + rows,)),
            dma((2,)),
            dma((2 * n,)),
            dma((4,)),
            dma((4,)),
        ],
        compiler_params=pltpu.CompilerParams(
            collective_id=0, has_side_effects=True, vmem_limit_bytes=56 << 20
        ),
        name="mixer",
    )(*args)


def state_kernel(
    sx_ref, dec_ref, bc_ref, fresh_ref, conv_ref, layer_ref, st_ref, out_ref, conv_out, lay, e_ref
):
    s = pl.program_id(0)
    rows = layer_ref.shape[0]
    blocks = HEAD_DIM * STATE // 256

    @pl.when(s == 0)
    def _():
        held = conv_ref.shape[0]
        for k in range(1, held):
            conv_out[k - 1] = conv_ref[k]
        conv_out[held - 1] = fresh_ref[...][:rows]
        lay[...] = layer_ref[...]

        def make(k, carry):
            at = pl.ds(pl.multiple_of(k * 256, 256), 256)
            p_of = iota((128, 256), 1) // STATE + 4 * k
            e_ref[:, at] = onehot(p_of == lax.rem(iota((128, 256), 0), HEAD_DIM))
            return carry

        lax.fori_loop(0, blocks, make, 0)

    sx = sx_ref[...]
    high = sx.astype(BF16).astype(F32)
    low = pltpu.roll(sx - high, HEAD_DIM, 1)
    lhs = jnp.where(iota((HEADS, 128), 1) < HEAD_DIM, high, low).astype(BF16)
    dec = dec_ref[...]
    row = bc_ref[pl.ds(s, 1), :]
    per = HEADS // SSM_GROUPS
    bs = []
    for g in range(SSM_GROUPS):
        b = row[:, g * STATE : (g + 1) * STATE]
        bs.append(jnp.broadcast_to(jnp.concatenate([b, b], axis=1), (per, 2 * STATE)))
    b_all = jnp.concatenate(bs, axis=0)
    for k in range(blocks):
        grown = dot(lhs, e_ref[:, k * 256 : (k + 1) * 256])
        for i in range(2):
            at = slice((2 * k + i) * 128, (2 * k + i + 1) * 128)
            out_ref[0, :, at] = dec * st_ref[0, :, at] + grown[:, i * 128 : (i + 1) * 128] * b_all


def state_update(sx, dec, bc, fresh, conv_t, layer, state_in):
    rows, _, flat = state_in.shape

    def whole(x):
        return pl.BlockSpec(x.shape, lambda s: (0,) * len(x.shape))

    part = pl.BlockSpec((HEADS, 128), lambda s: (s, 0))
    block = pl.BlockSpec((1, HEADS, flat), lambda s: (s, 0, 0))
    return pl.pallas_call(
        state_kernel,
        grid=(rows,),
        out_shape=(
            jax.ShapeDtypeStruct(state_in.shape, F32),
            jax.ShapeDtypeStruct(conv_t.shape, BF16),
            jax.ShapeDtypeStruct(layer.shape, BF16),
        ),
        in_specs=[part, part, whole(bc), whole(fresh), whole(conv_t), whole(layer), block],
        out_specs=(block, whole(conv_t), whole(layer)),
        scratch_shapes=[pltpu.VMEM((128, flat), BF16)],
        compiler_params=pltpu.CompilerParams(vmem_limit_bytes=24 << 20),
        name="state",
    )(sx, dec, bc, fresh, conv_t, layer, state_in)


def body(
    hidden,
    state_in,
    conv_state,
    expert_ids,
    group_prob,
    expert_score,
    first_gain,
    z_weight,
    x_weight,
    b_weight,
    c_weight,
    dt_weight,
    conv_weight,
    conv_bias,
    dt_bias,
    decay_log,
    skip_gain,
    inner_gain,
    out_weight,
    second_gain,
    expert_gate,
    expert_up,
    expert_down,
):
    n = lax.axis_size("ep")
    rows, width = hidden.shape
    cap = max(2, (3 * rows * TOP + 2 * n - 1) // (2 * n))
    conv_t = conv_state.transpose(1, 0, 2)
    args = (
        hidden,
        expert_ids.T,
        group_prob[None, :],
        expert_score.T,
        conv_t,
        conv_weight,
        conv_bias.reshape(-1, 128),
        first_gain.reshape(-1, 128),
        inner_gain.reshape(-1, 128),
        second_gain.reshape(-1, 128),
        dt_bias[None, :],
        decay_log[None, :],
        skip_gain[None, :],
        z_weight,
        x_weight,
        b_weight,
        c_weight,
        dt_weight.T,
        out_weight,
        expert_gate,
        expert_up,
        expert_down,
        state_in,
    )
    layer, sx, dec, bc, fresh = mixer(
        n, cap, args, rows, width, z_weight, out_weight, expert_gate, expert_down
    )
    state_out, conv_out, layer_out = state_update(sx, dec, bc, fresh, conv_t, layer, state_in)
    return (layer_out, state_out, conv_out.transpose(1, 0, 2))


def solution(mesh):
    in_specs = (
        P(("grp", "ep"), None),
        P(("grp", "ep"), None, None),
        P(("grp", "ep"), None, None),
        P(("grp", "ep"), None),
        P(("grp", "ep")),
        P(("grp", "ep"), None),
        P(),
        P(None, "ep"),
        P(None, "ep"),
        P(),
        P(),
        P(),
        P(),
        P(),
        P(),
        P(),
        P(),
        P(),
        P(None, "ep"),
        P(),
        P("ep", None, None),
        P("ep", None, None),
        P("ep", None, None),
    )
    out_specs = (P(("grp", "ep"), None), P(("grp", "ep"), None, None), P(("grp", "ep"), None, None))
    return jax.shard_map(body, mesh=mesh, in_specs=in_specs, out_specs=out_specs, check_vma=False)
```

```python
import functools

import jax
import jax.numpy as jnp
from jax import lax
from jax.experimental import pallas as pl
from jax.experimental.pallas import tpu as pltpu
from jax.sharding import PartitionSpec as P

HEADS = 64
HEAD_DIM = 64
SSM_GROUPS = 4
STATE = 64
TOP = 4
EPS = 1e-06
MESH = pl.DeviceIdType.MESH
F32 = jnp.float32
BF16 = jnp.bfloat16
ROWS = 8
INNER = HEADS * HEAD_DIM
SPAN = SSM_GROUPS * STATE


def rms_scale(values, gain_vec):
    return (
        values
        * lax.rsqrt(jnp.mean(values * values, axis=-1, keepdims=True) + EPS)
        * gain_vec.astype(F32)
    )


def dot(a, b):
    return jnp.dot(a, b, preferred_element_type=F32)


def dot_nt(a, b):
    return lax.dot_general(a, b, (((1,), (1,)), ((), ())), preferred_element_type=F32)


def iota(shape, axis):
    return lax.broadcasted_iota(jnp.int32, shape, axis)


def onehot(mask):
    return mask.astype(F32).astype(BF16)


def peer(index):
    return (lax.axis_index("grp"), index)


def remote(src, dst, send_sem, recv_sem, index):
    return pltpu.make_async_remote_copy(
        src_ref=src,
        dst_ref=dst,
        send_sem=send_sem,
        recv_sem=recv_sem,
        device_id=peer(index),
        device_id_type=MESH,
    )


def spread(ref):
    value = ref[...].astype(F32)
    return jnp.concatenate([value[i : i + 1] for i in range(value.shape[0])], axis=1)


def column(row):
    size = row.shape[1]
    at = iota((size, size), 0)
    to = iota((size, size), 1)
    return jnp.sum(jnp.where(at == to, row, jnp.zeros_like(row)), axis=1, keepdims=True)


class Gather:
    def __init__(self, n, buf, send, recv, split=1, direct=False):
        self.n, self.buf, self.send, self.recv = n, buf, send, recv
        self.split, self.direct = split, direct
        self.size = buf.shape[1] // split
        self.me = lax.axis_index("ep")
        self.outer = n // 4
        core = lax.rem(self.me, 2)
        mid = lax.rem(self.me // 2, 2)
        self.mate = self.me + 1 - 2 * core
        self.across = self.me + 2 - 4 * mid

    def at(self, k):
        return pl.ds(k * self.size, self.size)

    def sem(self, kind, d, k):
        return self.recv.at[(kind * self.outer + d) * self.split + k]

    def go(self, src, block, kind, d, k, to):
        dst = self.buf.at[block, self.at(k)]
        remote(src, dst, self.send.at[0], self.sem(kind, d, k), to).start()

    def arrive(self, block, kind, d, k):
        piece = self.buf.at[block, self.at(k)]
        remote(piece, piece, self.send.at[0], self.sem(kind, d, k), self.mate).wait_recv()

    def start(self, src):
        for k in range(self.split):
            piece = src.at[self.at(k)]
            for d in range(1, self.outer):
                far = lax.rem(self.across + 4 * d, self.n)
                if self.direct:
                    self.go(piece, self.me, 1, d, k, far)
                self.go(piece, self.me, 0, d, k, lax.rem(self.me + 4 * d, self.n))
            self.go(piece, self.me, 1, 0, k, self.across)
            self.go(piece, self.me, 2, 0, k, self.mate)

    def near(self, d):
        return lax.rem(self.me + self.n - 4 * d, self.n)

    def far(self, d):
        return lax.rem(self.across + self.n - 4 * d, self.n)

    def middle(self):
        for k in range(self.split):
            for d in range(1, self.outer):
                block = self.near(d)
                self.arrive(block, 0, d, k)
                piece = self.buf.at[block, self.at(k)]
                if not self.direct:
                    self.go(piece, block, 1, d, k, self.across)
                self.go(piece, block, 2, d, k, self.mate)

    def last(self):
        for k in range(self.split):
            for d in range(self.outer):
                block = self.far(d)
                self.arrive(block, 1, d, k)
                self.go(self.buf.at[block, self.at(k)], block, 3, d, k, self.mate)

    def finish(self, kind):
        for k in range(self.split):
            for d in range(self.outer):
                self.arrive(self.me, kind, d, k)

    def drain(self):
        piece = self.buf.at[pl.ds(0, self.n - 1)]
        remote(piece, piece, self.send.at[0], self.recv.at[0], self.mate).wait_send()


class Exchange:
    def __init__(self, n, out_buf, in_buf, send, recv, planes=False):
        self.n, self.out_buf, self.in_buf, self.send, self.recv = n, out_buf, in_buf, send, recv
        self.me = lax.axis_index("ep")
        self.z = self.me // 4
        self.w = lax.rem(self.me, 4)
        self.half = n // 8
        self.a = self.z // self.half
        self.b = lax.rem(self.z, self.half)
        self.planes = planes

    def order(self):
        near = [self.a * self.half + lax.rem(self.b + i, self.half) for i in range(self.half)]
        far = [(1 - self.a) * self.half + lax.rem(self.b + i, self.half) for i in range(self.half)]
        return near + far

    def start(self):
        sem = self.recv.at[self.z] if self.planes else self.recv.at[0]
        own, *near = self.order()
        for plane in near[self.half - 1 :] + near[: self.half - 1] + [own]:
            for i in range(4):
                if plane is own and i == 0:
                    continue
                to = 4 * plane + lax.rem(self.w + i, 4)
                remote(
                    self.out_buf.at[to], self.in_buf.at[self.me], self.send.at[0], sem, to
                ).start()
        self.in_buf[self.me] = self.out_buf[self.me]

    def _some(self, count, sem):
        part = pl.ds(0, count)
        return remote(self.out_buf.at[part], self.in_buf.at[part], self.send.at[0], sem, self.me)

    def wait(self):
        self._some(self.n - 1, self.recv.at[0]).wait_recv()

    def wait_plane(self, index, plane):
        self._some(3 if index == 0 else 4, self.recv.at[plane]).wait_recv()

    def drain(self):
        self._some(self.n - 1, self.recv.at[0]).wait_send()


def mixer_kernel(n, cap, *refs):
    (
        own_any,
        ids_any,
        prob_any,
        score_any,
        conv_any,
        taps_any,
        bias_any,
        g1_any,
        gi_any,
        g2_any,
        dtb_any,
        dlog_any,
        skip_any,
        z_any,
        x_any,
        b_any,
        c_any,
        dt_any,
        ow_any,
        eg_any,
        eu_any,
        ed_any,
        st_any,
        st,
        out_ref,
        fresh_ref,
        own_ref,
        ids_ref,
        prob_ref,
        score_ref,
        conv_ref,
        taps_ref,
        bias_ref,
        g1_ref,
        gi_ref,
        g2_ref,
        dtb_ref,
        dlog_ref,
        skip_ref,
        hid,
        hbuf,
        hall,
        hg,
        hsq,
        zw,
        xw,
        bw,
        cw,
        dw,
        ow,
        eg,
        eu,
        ed,
        prod,
        fold,
        grow,
        r0s,
        stepx,
        decx,
        sxs,
        bcs,
        cpart,
        pre_out,
        pre_in,
        x_out,
        x_in,
        yown,
        ybuf,
        igain,
        sel,
        bigh,
        bigl,
        hsel,
        p_out,
        p_in,
        mg,
        stage,
        spot_rows,
        o_out,
        o_in,
        wsem,
        gs,
        hr,
        yr,
        as_,
        ar,
        pr,
    ) = refs
    rows, width = own_ref.shape
    cols = zw.shape[1]
    ncol = ow.shape[1]
    total = n * ROWS
    slots = n * cap
    sp = sel.shape[0] // n
    chunks = width // 128
    per = HEADS // SSM_GROUPS
    me = lax.axis_index("ep")

    pairs = [
        (own_any, own_ref),
        (ids_any, ids_ref),
        (g1_any, g1_ref),
        (conv_any, conv_ref),
        (taps_any, taps_ref),
        (bias_any, bias_ref),
        (dtb_any, dtb_ref),
        (dlog_any, dlog_ref),
        (skip_any, skip_ref),
        (b_any, bw),
        (c_any, cw),
        (dt_any, dw),
        (gi_any, gi_ref),
        (g2_any, g2_ref),
        (prob_any, prob_ref),
        (score_any, score_ref),
        (x_any, xw),
        (z_any, zw),
        (ow_any, ow),
        (eg_any.at[0], eg),
        (eu_any.at[0], eu),
        (ed_any.at[0], ed),
    ]
    pairs += [(st_any.at[t], st.at[t]) for t in range(rows)]
    small, inputs, rest = 2, 12, 22
    loads = [pltpu.make_async_copy(src, dst, wsem.at[i]) for i, (src, dst) in enumerate(pairs)]
    for load in loads[:inputs] + loads[rest:] + loads[inputs:rest]:
        load.start()

    barrier = pltpu.get_barrier_semaphore()
    for d in range(1, n):
        pl.semaphore_signal(
            barrier, inc=1, device_id=peer(lax.rem(me + d, n)), device_id_type=MESH
        )
    for load in loads[:small]:
        load.wait()
    ids = ids_ref[...].astype(F32)
    pick = iota((TOP, 128), 0)
    lane = iota((TOP, 128), 1)
    spot = jnp.zeros((TOP, 128), F32)
    for r in range(rows):
        spot = spot + jnp.where(lane == TOP * r + pick, ids[:, r : r + 1] + 1.0, 0.0)
    id_row = jnp.sum(spot, axis=0, keepdims=True) - 1.0
    id_row = jnp.concatenate([id_row, jnp.full((1, width - 128), -1.0, F32)], axis=1)
    hid[...] = jnp.concatenate([own_ref[...].astype(F32), id_row], axis=0).astype(BF16)
    pl.semaphore_wait(barrier, n - 1)

    hidden_ag = Gather(n, hbuf, gs.at[pl.ds(0, 1)], hr, direct=True)
    hidden_ag.start(hid)
    hbuf[me] = hid[...]

    for load in loads[small:inputs]:
        load.wait()
    gain1 = spread(g1_ref)
    own = hid[...].astype(F32)
    mine = rms_scale(own, gain1).astype(BF16)
    taps = taps_ref[...].astype(F32)
    held = conv_ref.shape[0]
    summed = spread(bias_ref)
    for k in range(held):
        summed = summed + conv_ref[k].astype(F32) * taps[k : k + 1]
    cpart[...] = jnp.concatenate([summed, jnp.zeros((ROWS - rows, summed.shape[1]), F32)], axis=0)
    fresh_b = dot(mine, bw[...]).astype(BF16)
    fresh_c = dot(mine, cw[...]).astype(BF16)
    fresh_ref[:, INNER : INNER + SPAN] = fresh_b
    fresh_ref[:, INNER + SPAN :] = fresh_c
    b_act = jax.nn.silu(
        cpart[:, INNER : INNER + SPAN]
        + fresh_b.astype(F32) * taps[held : held + 1, INNER : INNER + SPAN]
    )
    c_act = jax.nn.silu(
        cpart[:, INNER + SPAN :] + fresh_c.astype(F32) * taps[held : held + 1, INNER + SPAN :]
    )
    bcs[:, :SPAN] = b_act
    bcs[:, SPAN:] = c_act
    dt = dot_nt(mine, dw[...]).astype(BF16).astype(F32)
    step = jax.nn.softplus(dt + dtb_ref[...])
    dt_t = dot_nt(dw[...], mine).astype(BF16).astype(F32)
    step_t = jax.nn.softplus(dt_t + column(dtb_ref[...]))
    decay_t = jnp.exp(-step_t * jnp.exp(column(dlog_ref[...])))
    for t in range(rows):
        at = slice(t * HEADS, (t + 1) * HEADS)
        stepx[at, :] = jnp.broadcast_to(step_t[:, t : t + 1], (HEADS, 128))
        decx[at, :] = jnp.broadcast_to(decay_t[:, t : t + 1], (HEADS, 128))
    pad = slice(rows * HEADS, ROWS * HEADS)
    stepx[pad, :] = jnp.zeros(((ROWS - rows) * HEADS, 128), F32)
    decx[pad, :] = jnp.zeros(((ROWS - rows) * HEADS, 128), F32)
    r0s[pad, :] = jnp.zeros(((ROWS - rows) * HEADS, 128), F32)
    bc = b_act * c_act
    bc_hi = bc.astype(BF16)
    bc_lo = (bc - bc_hi.astype(F32)).astype(BF16)
    group = onehot(iota((SPAN, 128), 0) // STATE == iota((SPAN, 128), 1) // per)
    inner = dot(bc_hi, group) + dot(bc_lo, group)
    coef = step * inner[:, :HEADS] + skip_ref[...]
    row_ok = iota((ROWS, HEADS), 0) < rows
    coef = jnp.where(row_ok, coef, 0.0)
    coef = jnp.concatenate([coef, jnp.zeros((ROWS, 128 - HEADS), F32)], axis=1).astype(BF16)

    def make_fold(i, carry):
        at = pl.ds(pl.multiple_of(i * 256, 256), 256)
        p_of = iota((256, 128), 0) // STATE + 4 * i
        fold[at, :] = onehot(p_of == lax.rem(iota((256, 128), 1), HEAD_DIM))
        return carry

    lax.fori_loop(0, INNER // 256, make_fold, 0)

    def make_prod(t, carry):
        pltpu.make_async_copy(st_any.at[t], st.at[t], wsem.at[rest + t]).wait()
        row = bcs[pl.ds(t, 1), :]
        cs = []
        for g in range(SSM_GROUPS):
            c = row[:, SPAN + g * STATE : SPAN + (g + 1) * STATE]
            cs.append(jnp.broadcast_to(jnp.concatenate([c, c], axis=1), (per, 2 * STATE)))
        c_all = jnp.concatenate(cs, axis=0)
        at = pl.ds(pl.multiple_of(t * HEADS, HEADS), HEADS)
        for k in range(HEAD_DIM * STATE // 128):
            lanes = slice(k * 128, (k + 1) * 128)
            prod[at, lanes] = (st[t, :, lanes] * c_all).astype(BF16)
        return carry

    lax.fori_loop(0, rows, make_prod, 0)
    cut = (rows + 1) // 2 * HEADS
    for at in (slice(0, cut), slice(cut, rows * HEADS)):
        r0s[at, :] = dot(prod[at, :], fold[...]) * decx[at, :]
    low_half = iota((ROWS, 128), 1) < HEAD_DIM
    for m in range(INNER // 128):
        even = r0s[pl.ds(2 * m, ROWS, stride=HEADS), :]
        odd = r0s[pl.ds(2 * m + 1, ROWS, stride=HEADS), :]
        j, off = (m * 128) // cols, (m * 128) % cols
        pre_out[j, :, off : off + 128] = jnp.where(low_half, even, odd).astype(BF16)
    for j in range(n):
        pre_out[j, :, cols : 2 * cols] = cpart[:, j * cols : (j + 1) * cols].astype(BF16)
        pre_out[j, :, 2 * cols :] = coef
    pre = Exchange(n, pre_out, pre_in, as_.at[pl.ds(0, 1)], ar.at[pl.ds(0, 1)])
    pre.start()
    hidden_ag.middle()
    hidden_ag.last()
    for load in loads[inputs : inputs + 6]:
        load.wait()
    hidden_ag.finish(2)
    hidden_ag.finish(3)
    for j in range(0, n, 2):
        at = slice(j * ROWS, (j + 2) * ROWS)
        pair = jnp.concatenate([hbuf[j].astype(F32), hbuf[j + 1].astype(F32)], axis=0)
        hall[at, :] = pair.astype(BF16)
        hg[at, :] = (pair * gain1).astype(BF16)
        hsq[at, :] = (pair * pair).astype(BF16)
    ones = jnp.ones((width, 128), BF16)
    scale = lax.rsqrt(dot(hsq[...], ones) * (1.0 / width) + EPS)
    scale = jnp.concatenate([scale] * (cols // 128), axis=1)
    xp = (dot(hg[...], xw[...]) * scale).astype(BF16).astype(F32)
    zp = (dot(hg[...], zw[...]) * scale).astype(BF16).astype(F32)
    for j in range(n):
        x_out[j] = xp[j * ROWS : (j + 1) * ROWS].astype(BF16)
    my_cols = pl.ds(pl.multiple_of(me * cols, 128), cols)
    tap = taps_ref[:, my_cols].astype(F32)[held : held + 1]
    gain_all = spread(gi_ref)
    cpart_gain = jnp.broadcast_to(gain_all, (ROWS, INNER))
    stage[pl.ds(0, ROWS), :] = cpart_gain[:, :width]
    stage[pl.ds(ROWS, ROWS), :] = cpart_gain[:, width:]
    half_n = n // 2
    upper = me // half_n
    gain_cols = stage[
        pl.ds(pl.multiple_of(upper * ROWS, ROWS), ROWS),
        pl.ds(pl.multiple_of(lax.rem(me, half_n) * cols, 128), cols),
    ]
    pre.wait()
    for j in range(0, n, 2):
        ys = []
        for i in (j, j + 1):
            at = slice(i * ROWS, (i + 1) * ROWS)
            block = pre_in[i].astype(F32)
            xa = jax.nn.silu(block[:, cols : 2 * cols] + xp[at] * tap)
            packed = block[:, 2 * cols :]
            grown = []
            for k in range(cols // 128):
                index = (me * cols + k * 128) // HEAD_DIM + iota((ROWS, 128), 1) // HEAD_DIM
                grown.append(jnp.take_along_axis(packed, index, axis=1))
            readout = block[:, :cols] + jnp.concatenate(grown, axis=1) * xa
            ys.append(readout * jax.nn.silu(zp[at]) * gain_cols)
        yown[j * ROWS : (j + 2) * ROWS, :] = jnp.concatenate(ys, axis=0).astype(BF16)

    y_ag = Gather(n, ybuf, gs.at[pl.ds(1, 1)], yr, split=2)
    y_ag.start(yown)
    ybuf[me] = yown[...]
    igain[...] = jnp.broadcast_to(1.0 / gain_all, igain.shape)
    ones_c = jnp.ones((cols, 128), BF16)

    def project(blocks, acc, ssq):
        for block in blocks:
            lanes = pl.ds(pl.multiple_of(block * cols, 128), cols)
            yb = ybuf[block]
            acc = acc + dot(yb, ow[lanes, :])
            inv = jnp.concatenate([igain[:, lanes]] * n, axis=0)
            raw = yb.astype(F32) * inv
            ssq = ssq + dot((raw * raw).astype(BF16), ones_c)
        return acc, ssq

    q = iota((slots, total), 0)
    t_of = iota((slots, total), 1)
    last = onehot(t_of == lax.rem(q, n) * ROWS + (ROWS - 1))
    id_all = dot(last, hall[:, :128])
    f_lane = iota((128, total), 0) // TOP
    token = lax.rem(iota((128, total), 1), ROWS)
    m_here = onehot(f_lane == token)
    m_less = onehot(f_lane < token)
    flags = jnp.concatenate([onehot(id_all == float(e)) for e in range(n)], axis=0)
    here = dot(flags, m_here)
    before = dot(flags, m_less)
    same = lax.rem(q, n) == t_of // ROWS
    rank_q = (q // n).astype(F32)
    own_row = iota((ROWS, total), 0)
    own_col = iota((ROWS, total), 1)
    for e in range(n):
        at = slice(e * slots, (e + 1) * slots)
        chosen = same & (here[at] > 0.5) & (before[at] == rank_q)
        tail = [(own_col == e * ROWS + own_row).astype(F32)]
        if sp > slots + ROWS:
            tail.append(jnp.zeros((sp - slots - ROWS, total), F32))
        sel[e * sp : (e + 1) * sp, :] = jnp.concatenate(
            [chosen.astype(F32)] + tail, axis=0
        ).astype(BF16)

    y_ag.middle()
    near = [me] + [y_ag.near(d) for d in range(1, n // 4)]
    acc = jnp.zeros((total, ncol), F32)
    ssq = jnp.zeros((total, 128), F32)
    loads[inputs + 6].wait()
    acc, ssq = project(near, acc, ssq)

    span = chunks * cap
    wide = n * span
    col = iota((rows, wide), 1).astype(F32)
    e_of = jnp.floor((col + 0.5) * (1.0 / span))
    in_e = col - e_of * span
    k_of = jnp.floor((in_e + 0.5) * (1.0 / cap))
    r_of = in_e - k_of * cap
    score = score_ref[...]
    share = prob_ref[...] * score / jnp.sum(score, axis=0, keepdims=True)
    weight = jnp.zeros((rows, wide), F32)
    used = jnp.zeros((rows, wide), F32)
    for i in range(TOP):
        hit = (column(ids[i : i + 1]) == e_of).astype(F32)
        used = used + hit
        weight = weight + hit * column(share[i : i + 1])
    row_id = iota((rows, wide), 0)
    rank = jnp.zeros((rows, wide), F32)
    for r in range(rows - 1):
        rank = rank + jnp.where(row_id > r, used[r : r + 1, :], 0.0)
    weight = jnp.where(rank == r_of, weight, 0.0)
    weight = jnp.concatenate([weight, jnp.zeros((ROWS - rows, wide), F32)], axis=0)
    k_row = k_of[0:1]
    for k in range(0, chunks, 2):
        both = jnp.concatenate(
            [jnp.where(k_row == float(k + i), weight, 0.0) for i in range(2)], axis=0
        )
        high = both.astype(BF16)
        at = slice(k * ROWS, (k + 2) * ROWS)
        bigh[at, :] = high
        bigl[at, :] = (both - high.astype(F32)).astype(BF16)
    pick_me = sel[pl.ds(pl.multiple_of(me * sp, 16), sp), :][:slots]
    hsel[...] = dot(pick_me, hall[...])

    y_ag.last()

    back = Exchange(n, x_out, x_in, as_.at[pl.ds(1, 1)], ar.at[pl.ds(1, 1)])
    back.start()
    far = [y_ag.far(d) for d in range(n // 4)]
    acc, ssq = project(far, acc, ssq)
    shift = y_ag.mate - me
    y_ag.finish(2)
    acc, ssq = project([block + shift for block in near], acc, ssq)
    y_ag.finish(3)
    acc, ssq = project([block + shift for block in far], acc, ssq)
    scale = lax.rsqrt(ssq * (1.0 / INNER) + EPS)
    p = (acc * scale[:, :ncol]).astype(BF16)
    picked = dot(sel[...], p).astype(BF16)
    for e in range(n):
        p_out[e] = picked[e * sp : e * sp + slots + ROWS]
    p_ex = Exchange(n, p_out, p_in, as_.at[pl.ds(2, 1)], pr, planes=True)
    p_ex.start()

    back.wait()
    for j in range(n):
        xv = x_in[j]
        fresh_ref[:, j * cols : (j + 1) * cols] = xv
        at = slice(j * cols, (j + 1) * cols)
        xa = jax.nn.silu(cpart[:, at] + xv.astype(F32) * taps_ref[held : held + 1, at].astype(F32))
        for k in range(cols // 128):
            m = (j * cols) // 128 + k
            piece = xa[:, k * 128 : (k + 1) * 128]
            sxs[pl.ds(2 * m, ROWS, stride=HEADS), :] = piece
            sxs[pl.ds(2 * m + 1, ROWS, stride=HEADS), :] = pltpu.roll(piece, HEAD_DIM, 1)
    for load in loads[inputs + 7 : rest]:
        load.wait()

    gain2 = spread(g2_ref)
    ssq = jnp.zeros((slots, 128), F32)
    ones_n = jnp.ones((ncol, 128), BF16)
    band = 4 * ncol
    units = eg.shape[1]
    stage[:ROWS, :] = jnp.broadcast_to(gain2, (ROWS, width))
    stage[ROWS:, :] = own
    gate = jnp.zeros((slots, units), F32)
    up = jnp.zeros((slots, units), F32)
    for i, plane in enumerate(p_ex.order()):
        p_ex.wait_plane(i, plane)
        at = pl.ds(pl.multiple_of(plane * band, 128), band)
        block = jnp.concatenate([p_in[4 * plane + w].astype(F32) for w in range(4)], axis=1)
        m = (hsel[:, at] + block[:slots]).astype(BF16).astype(F32)
        scaled = (m * stage[0:1, at]).astype(BF16)
        square = (m * m).astype(BF16)
        for w in range(4):
            ssq = ssq + dot(square[:, w * ncol : (w + 1) * ncol], ones_n)
        gate = gate + dot(scaled, eg[at, :])
        up = up + dot(scaled, eu[at, :])
        stage[ROWS:, at] = (stage[ROWS:, at] + block[slots:]).astype(BF16).astype(F32)
    scale = lax.rsqrt(ssq * (1.0 / width) + EPS)
    acts = []
    for j in range(0, units, 128):
        at = slice(j, j + 128)
        acts.append((jax.nn.silu(gate[:, at] * scale) * (up[:, at] * scale)).astype(BF16))
    act = jnp.concatenate(acts, axis=1)
    for k in range(0, chunks, 2):
        part = dot(act, ed[:, k * 128 : (k + 2) * 128])
        for i in range(2):
            for r in range(cap):
                spot_rows[pl.ds((k + i) * cap + r, n, stride=span), :] = part[
                    r * n : (r + 1) * n, i * 128 : (i + 1) * 128
                ]
    for s in range(n):
        o_out[s] = spot_rows[s * span : (s + 1) * span, :].astype(BF16)
    o_ex = Exchange(n, o_out, o_in, as_.at[pl.ds(3, 1)], ar.at[pl.ds(3, 1)])
    o_ex.start()

    def make_grow(i, carry):
        at = pl.ds(pl.multiple_of(i * 256, 256), 256)
        p_of = iota((128, 256), 1) // STATE + 4 * i
        grow[:, at] = onehot(p_of == lax.rem(iota((128, 256), 0), HEAD_DIM))
        return carry

    lax.fori_loop(0, HEAD_DIM * STATE // 256, make_grow, 0)

    def update(t, carry):
        at = pl.ds(pl.multiple_of(t * HEADS, HEADS), HEADS)
        sx = sxs[at, :] * stepx[at, :]
        high = sx.astype(BF16).astype(F32)
        low = pltpu.roll(sx - high, HEAD_DIM, 1)
        lhs = jnp.where(iota((HEADS, 128), 1) < HEAD_DIM, high, low).astype(BF16)
        dec = decx[at, :]
        row = bcs[pl.ds(t, 1), :]
        bs = []
        for g in range(SSM_GROUPS):
            b = row[:, g * STATE : (g + 1) * STATE]
            bs.append(jnp.broadcast_to(jnp.concatenate([b, b], axis=1), (per, 2 * STATE)))
        b_all = jnp.concatenate(bs, axis=0)
        for k in range(HEAD_DIM * STATE // 256):
            grown = dot(lhs, grow[:, k * 256 : (k + 1) * 256])
            for i in range(2):
                lanes = slice((2 * k + i) * 128, (2 * k + i + 1) * 128)
                term = grown[:, i * 128 : (i + 1) * 128] * b_all
                st[t, :, lanes] = dec * st[t, :, lanes] + term
        return carry

    lax.fori_loop(0, rows, update, 0)
    hidden_ag.drain()
    y_ag.drain()
    pre.drain()
    back.drain()
    p_ex.drain()
    o_ex.wait()
    got = jnp.concatenate([o_in[e] for e in range(n)], axis=0)
    moe = dot(bigh[...], got) + dot(bigl[...], got)
    for k in range(chunks):
        at = slice(k * 128, (k + 1) * 128)
        out_ref[:, at] = (stage[ROWS:, at] + moe[k * ROWS : (k + 1) * ROWS])[:rows].astype(BF16)
    o_ex.drain()


def mixer(n, cap, args, rows, width, z_weight, out_weight, expert_gate, expert_down):
    cols = z_weight.shape[1]
    ncol = out_weight.shape[1]
    units = expert_gate.shape[2]
    total = n * ROWS
    slots = n * cap
    sp = (slots + ROWS + 15) // 16 * 16
    chunks = width // 128
    span = chunks * cap
    vm = pl.BlockSpec(memory_space=pltpu.VMEM)
    hbm = pl.BlockSpec(memory_space=pl.ANY)
    dma = pltpu.SemaphoreType.DMA

    def buf(*shape, dtype=BF16):
        return pltpu.VMEM(shape, dtype)

    return pl.pallas_call(
        functools.partial(mixer_kernel, n, cap),
        out_shape=(
            pltpu.VMEM((rows, HEADS, HEAD_DIM * STATE), F32),
            pltpu.VMEM((rows, width), BF16),
            pltpu.VMEM((ROWS, INNER + 2 * SPAN), BF16),
        ),
        in_specs=[hbm] * 23,
        out_specs=(vm,) * 3,
        scratch_shapes=[pltpu.VMEM(x.shape, x.dtype) for x in args[:13]]
        + [
            buf(ROWS, width),
            buf(n, ROWS, width),
            buf(total, width),
            buf(total, width),
            buf(total, width),
            buf(width, cols),
            buf(width, cols),
            buf(width, SPAN),
            buf(width, SPAN),
            buf(HEADS, width),
            buf(INNER, ncol),
            buf(width, units),
            buf(width, units),
            buf(units, width),
            buf(rows * HEADS, HEAD_DIM * STATE),
            buf(INNER, 128),
            buf(128, HEAD_DIM * STATE),
            buf(ROWS * HEADS, 128, dtype=F32),
            buf(ROWS * HEADS, 128, dtype=F32),
            buf(ROWS * HEADS, 128, dtype=F32),
            buf(ROWS * HEADS, 128, dtype=F32),
            buf(ROWS, 2 * SPAN, dtype=F32),
            buf(ROWS, INNER + 2 * SPAN, dtype=F32),
            buf(n, ROWS, 2 * cols + 128),
            buf(n, ROWS, 2 * cols + 128),
            buf(n, ROWS, cols),
            buf(n, ROWS, cols),
            buf(total, cols),
            buf(n, total, cols),
            buf(ROWS, INNER, dtype=F32),
            buf(n * sp, total),
            buf(chunks * ROWS, n * span),
            buf(chunks * ROWS, n * span),
            buf(slots, width, dtype=F32),
            buf(n, slots + ROWS, ncol),
            buf(n, slots + ROWS, ncol),
            buf(slots, width),
            buf(2 * ROWS, width, dtype=F32),
            buf(n * span, 128, dtype=F32),
            buf(n, span, 128),
            buf(n, span, 128),
            dma((22 + rows,)),
            dma((2,)),
            dma((n,)),
            dma((2 * n,)),
            dma((4,)),
            dma((4,)),
            dma((n // 4,)),
        ],
        compiler_params=pltpu.CompilerParams(
            collective_id=0, has_side_effects=True, vmem_limit_bytes=48 << 20
        ),
        name="mixer",
    )(*args)


def write_kernel(st_ref, layer_ref, fresh_ref, conv_ref, out_any, lay_any, conv_any, rows3, sem):
    rows = layer_ref.shape[0]
    held = conv_ref.shape[0]
    copies = [pltpu.make_async_copy(st_ref.at[t], out_any.at[t], sem.at[t]) for t in range(rows)]
    copies.append(pltpu.make_async_copy(layer_ref, lay_any, sem.at[rows]))
    for copy in copies:
        copy.start()
    for k in range(1, held):
        rows3[k - 1] = conv_ref[k]
    rows3[held - 1] = fresh_ref[...][:rows]
    copies.append(pltpu.make_async_copy(rows3, conv_any, sem.at[rows + 1]))
    copies[-1].start()
    for copy in copies:
        copy.wait()


def write(st, layer, fresh, conv_t):
    rows = layer.shape[0]
    vm = pl.BlockSpec(memory_space=pltpu.VMEM)
    hbm = pl.BlockSpec(memory_space=pl.ANY)
    return pl.pallas_call(
        write_kernel,
        out_shape=(
            jax.ShapeDtypeStruct(st.shape, F32),
            jax.ShapeDtypeStruct(layer.shape, BF16),
            jax.ShapeDtypeStruct(conv_t.shape, BF16),
        ),
        in_specs=[vm] * 4,
        out_specs=(hbm,) * 3,
        scratch_shapes=[
            pltpu.VMEM(conv_t.shape, BF16),
            pltpu.SemaphoreType.DMA((rows + 2,)),
        ],
        compiler_params=pltpu.CompilerParams(vmem_limit_bytes=4 << 20),
        name="write",
    )(st, layer, fresh, conv_t)


def body(
    hidden,
    state_in,
    conv_state,
    expert_ids,
    group_prob,
    expert_score,
    first_gain,
    z_weight,
    x_weight,
    b_weight,
    c_weight,
    dt_weight,
    conv_weight,
    conv_bias,
    dt_bias,
    decay_log,
    skip_gain,
    inner_gain,
    out_weight,
    second_gain,
    expert_gate,
    expert_up,
    expert_down,
):
    n = lax.axis_size("ep")
    rows, width = hidden.shape
    cap = max(2, (3 * rows * TOP + 2 * n - 1) // (2 * n))
    conv_t = conv_state.transpose(1, 0, 2)
    args = (
        hidden,
        expert_ids.T,
        group_prob[None, :],
        expert_score.T,
        conv_t,
        conv_weight,
        conv_bias.reshape(-1, 128),
        first_gain.reshape(-1, 128),
        inner_gain.reshape(-1, 128),
        second_gain.reshape(-1, 128),
        dt_bias[None, :],
        decay_log[None, :],
        skip_gain[None, :],
        z_weight,
        x_weight,
        b_weight,
        c_weight,
        dt_weight.T,
        out_weight,
        expert_gate,
        expert_up,
        expert_down,
        state_in,
    )
    st, layer, fresh = mixer(
        n, cap, args, rows, width, z_weight, out_weight, expert_gate, expert_down
    )
    state_out, layer_out, conv_out = write(st, layer, fresh, conv_t)
    return (layer_out, state_out, conv_out.transpose(1, 0, 2))


def solution(mesh):
    in_specs = (
        P(("grp", "ep"), None),
        P(("grp", "ep"), None, None),
        P(("grp", "ep"), None, None),
        P(("grp", "ep"), None),
        P(("grp", "ep")),
        P(("grp", "ep"), None),
        P(),
        P(None, "ep"),
        P(None, "ep"),
        P(),
        P(),
        P(),
        P(),
        P(),
        P(),
        P(),
        P(),
        P(),
        P(None, "ep"),
        P(),
        P("ep", None, None),
        P("ep", None, None),
        P("ep", None, None),
    )
    out_specs = (P(("grp", "ep"), None), P(("grp", "ep"), None, None), P(("grp", "ep"), None, None))
    return jax.shard_map(body, mesh=mesh, in_specs=in_specs, out_specs=out_specs, check_vma=False)
```
